32 devices in a mesh: ep: 16 (over z, y, x), tp: 2 (over core).
Axes of the slice: x: 2, y: 2, z: 4, core: 2. Of those that a mesh axis runs over, the one named last changes fastest.
Arguments:
- tokens: bfloat16 [256, 2048], P('ep'), may hold values from -6 to 6
- lengths: int32 [256], P('ep'), may hold values from 1 to 1024, as said below
- attn_gain: float32 [2048], replicated, may hold values from 0.1 to 1.9
- w_query: bfloat16 [2048, 1024], P(None, 'tp'), may hold values from -0.125 to 0.125
- w_key: bfloat16 [2048, 128], P(None, 'tp'), may hold values from -0.125 to 0.125
- w_value: bfloat16 [2048, 128], P(None, 'tp'), may hold values from -0.125 to 0.125
- head_bias: float32 [16], P('tp'), may hold values from -7 to -2
- key_cache: bfloat16 [256, 2, 64, 1024], P('ep', 'tp'), may hold values from -6 to 6
- value_cache: bfloat16 [256, 2, 64, 1024], P('ep', 'tp'), may hold values from -6 to 6
- w_attn_out: bfloat16 [1024, 2048], P('tp'), may hold values from -0.1875 to 0.1875
- ffn_gain: float32 [2048], replicated, may hold values from 0.1 to 1.9
- w_router: bfloat16 [2048, 16], replicated, may hold values from -0.125 to 0.125
- routes: int32 [256, 6], P('ep'), may hold values from 0 to 15, all different within a row; in each aligned block of 16 rows (0 to 15, 16 to 31, ...) at most 12 rows name the same one
- w_dense_gate: bfloat16 [2048, 512], P('ep', 'tp'), may hold values from -0.125 to 0.125
- w_dense_up: bfloat16 [2048, 512], P('ep', 'tp'), may hold values from -0.125 to 0.125
- w_dense_down: bfloat16 [512, 2048], P('tp', 'ep'), may hold values from -0.25 to 0.25
- dense_mix: float32 [2048], replicated, may hold values from -0.125 to 0.125
- w_expert_gate: bfloat16 [16, 2048, 512], P('ep', None, 'tp'), may hold values from -0.125 to 0.125
- w_expert_up: bfloat16 [16, 2048, 512], P('ep', None, 'tp'), may hold values from -0.125 to 0.125
- w_expert_down: bfloat16 [16, 512, 2048], P('ep', 'tp'), may hold values from -0.25 to 0.25
Outputs:
- layer_out: bfloat16 [256, 2048], P('ep', 'tp')
- new_keys: bfloat16 [256, 128], P('ep', 'tp')
- new_values: bfloat16 [256, 128], P('ep', 'tp')
The draws below stay inside these ranges and needn't reach their ends.
Inputs may be any that keep to these rules, and one draw needn't show every extreme that they name: `lengths`: every sequence holds between 1 and 1024 cached positions; in every draw some sequence holds exactly 1024. `routes`: each token names 6 different experts. Among the rows of one device no expert is named by more than 12 rows.
All inputs are finite; a program needn't handle non-finite values.
Results may differ from the reference program's by a relative error of at most 0.014.
Values may be sent and summed in bfloat16 or wider, within the bound.
A program may use at most 64 MiB of HBM per device.

```python
import math
import jax
import jax.numpy as jnp
import numpy as np
from jax import lax

D = 2048
HEADS = 16
KV_HEADS = 2
HEAD = 64
EXPERT_WIDTH = 512
SHARED = 512
TOP_K = 6
SEQ_DEV = 16
CACHE = 1024
EXPERTS = 16
TOKENS = 256
CAP = 12
N_EP = 16
N_TP = 2


def draw_lengths(key, part):
    key_caps = jax.random.fold_in(key, 11)
    key_rows = jax.random.fold_in(key, 12)
    key_full = jax.random.fold_in(key, 13)
    group_total = TOKENS // SEQ_DEV
    device_caps = jax.random.randint(key_caps, (group_total, 1), CACHE // 8, CACHE + 1)
    drawn = jax.random.randint(key_rows, (group_total, SEQ_DEV), 1, device_caps + 1).reshape(-1)
    full_at = jax.random.randint(key_full, (), 0, TOKENS)
    drawn = jnp.where(jnp.arange(TOKENS, dtype=jnp.int32) == full_at, CACHE, drawn)
    return drawn.astype(jnp.int32)


def levels(rng, shape, pieces, least, top_value):
    level, own = 1.0, jax.random.fold_in(rng, 6)
    for position, shards_of in pieces:
        steps = jnp.exp(jax.random.uniform(jax.random.fold_in(own, position), (shards_of,), jnp.float32, least / len(pieces), top_value / len(pieces)))
        level = level * jnp.repeat(steps, shape[position] // shards_of).reshape([-1 if axis == position else 1 for axis in range(len(shape))])
    return level


def shared_out(own_key, own, number, rows, number_of, top, limit, slope):
    order = jax.random.permutation(own_key, number_of)
    crowded, ordinary = shares(number_of, rows * top, limit, slope, True), shares(number_of, rows * top, limit, slope, False)
    places = jnp.arange(number_of)

    def named(sizes, rotation):
        used = int((sizes > 0).sum())
        fixed = max(1, used // 4)
        shifted = fixed + (places - fixed + rotation * (used - fixed)) % max(1, number_of - fixed)
        return jnp.zeros((number_of,), jnp.int32).at[order[jnp.where(places < fixed, places, shifted)]].set(jnp.asarray(sizes, jnp.int32))

    sizes = jnp.where(number % 4 == 0, named(crowded, number // 4), named(ordinary, number - number // 4 - 1))
    mixed = jax.random.permutation(jax.random.fold_in(own, 3), number_of)
    donor, taker = mixed[0:number_of // 2 * 2:2], mixed[1:number_of // 2 * 2:2]
    margin = jnp.minimum(sizes[donor] - 1, limit - sizes[taker]) // 2
    margin = jnp.where((donor == order[0]) | (taker == order[0]) | (sizes[taker] == 0), 0, jnp.maximum(margin, 0))
    shifted = jax.random.randint(jax.random.fold_in(own, 4), (number_of // 2,), 0, 1 << 20) % (margin + 1)
    sizes = sizes.at[donor].add(-shifted).at[taker].add(shifted)
    members = jnp.searchsorted(jnp.cumsum(sizes), jnp.arange(rows * top), side="right").astype(jnp.int32)
    listing = members.reshape(top, rows).T
    listing = listing[jax.random.permutation(jax.random.fold_in(own, 1), rows)]
    rotation = jax.random.randint(jax.random.fold_in(own, 2), (rows, 1), 0, top)
    return jnp.take_along_axis(listing, (jnp.arange(top)[None, :] + rotation) % top, axis=1)


def shares(number_of, total, most, skew, full):
    loads = [(1 << 20) // math.isqrt(standing ** skew) + 1 for standing in range(1, number_of + 1)]
    largest = most if full else min(most, max(-(-total // number_of), total * loads[0] // sum(loads)))
    least = 1 if total - largest >= number_of - 1 else 0
    given, rest = [largest] + [least] * (number_of - 1), total - largest - least * (number_of - 1)
    while rest > 0:
        free = [i for i in range(1, number_of) if given[i] < largest] or [i for i in range(1, number_of) if given[i] < most]
        mass, budget = sum([loads[i] for i in free]), rest
        for i in free:
            addition = min(most - given[i], max(1, budget * loads[i] // mass), rest)
            given[i] = given[i] + addition
            rest = rest - addition
    return np.array(given)


def gaussian(own_key, extent, spread, most, split=(), held_as=jnp.bfloat16):
    level = levels(own_key, extent, split, -0.22, 0.18) if split else 1.0
    entries = jax.random.normal(own_key, extent, jnp.float32) * spread * level
    return jnp.minimum(jnp.maximum(entries, -most), most).astype(held_as)


def setup_inputs(seed: int = 0) -> dict:
    streams_of = jax.random.split(jax.random.key(seed), 21)
    tokens = gaussian(streams_of[0], (TOKENS, D), 1.0, 6.0, ((0, 16),))
    lengths = draw_lengths(jax.random.fold_in(streams_of[20], 71), 0)
    attn_gain = jnp.clip(1.0 + 0.18 * jax.random.normal(streams_of[2], (D,), jnp.float32), 0.1, 1.9)
    w_query = gaussian(streams_of[3], (D, HEADS * HEAD), D ** -0.5, 0.125, ((1, 2),))
    w_key = gaussian(streams_of[4], (D, KV_HEADS * HEAD), D ** -0.5, 0.125, ((1, 2),))
    w_value = gaussian(streams_of[5], (D, KV_HEADS * HEAD), D ** -0.5, 0.125, ((1, 2),))
    head_bias = jnp.clip(-7.0 + 5.0 * jax.random.uniform(streams_of[6], (HEADS,), jnp.float32) ** levels(streams_of[6], (HEADS,), ((0, 2),), -0.2, 0.2), -7.0, -2.0)
    key_cache = gaussian(streams_of[7], (TOKENS, KV_HEADS, HEAD, CACHE), 1.0, 6.0, ((0, 16), (1, 2)))
    value_cache = gaussian(streams_of[8], (TOKENS, KV_HEADS, HEAD, CACHE), 1.0, 6.0, ((0, 16), (1, 2)))
    w_attn_out = gaussian(streams_of[9], (HEADS * HEAD, D), (HEADS * HEAD) ** -0.5, 0.1875, ((0, 2),))
    ffn_gain = jnp.clip(1.0 + 0.18 * jax.random.normal(streams_of[10], (D,), jnp.float32), 0.1, 1.9)
    w_router = gaussian(streams_of[11], (D, EXPERTS), D ** -0.5, 0.125)
    routes_keys = jax.random.split(jax.random.fold_in(streams_of[12], 1), TOKENS // SEQ_DEV)
    routes_turns = jax.random.permutation(jax.random.fold_in(streams_of[12], 3), TOKENS // SEQ_DEV)
    routes = jax.vmap(lambda own, number: shared_out(jax.random.fold_in(streams_of[12], 2), own, number, SEQ_DEV, EXPERTS, TOP_K, CAP, 2))(routes_keys, routes_turns).reshape((TOKENS, TOP_K))
    w_dense_gate = gaussian(streams_of[13], (D, SHARED), D ** -0.5, 0.125, ((0, 16), (1, 2)))
    w_dense_up = gaussian(streams_of[14], (D, SHARED), D ** -0.5, 0.125, ((0, 16), (1, 2)))
    w_dense_down = gaussian(streams_of[15], (SHARED, D), SHARED ** -0.5, 0.25, ((0, 2), (1, 16)))
    dense_mix = gaussian(streams_of[16], (D,), D ** -0.5, 0.125, (), jnp.float32)
    w_expert_gate = gaussian(streams_of[17], (EXPERTS, D, EXPERT_WIDTH), D ** -0.5, 0.125, ((0, 16), (2, 2)))
    w_expert_up = gaussian(streams_of[18], (EXPERTS, D, EXPERT_WIDTH), D ** -0.5, 0.125, ((0, 16), (2, 2)))
    w_expert_down = gaussian(streams_of[19], (EXPERTS, EXPERT_WIDTH, D), EXPERT_WIDTH ** -0.5, 0.25, ((0, 16), (1, 2)))
    return {"tokens": tokens, "lengths": lengths, "attn_gain": attn_gain, "w_query": w_query, "w_key": w_key, "w_value": w_value, "head_bias": head_bias, "key_cache": key_cache, "value_cache": value_cache, "w_attn_out": w_attn_out, "ffn_gain": ffn_gain, "w_router": w_router, "routes": routes, "w_dense_gate": w_dense_gate, "w_dense_up": w_dense_up, "w_dense_down": w_dense_down, "dense_mix": dense_mix, "w_expert_gate": w_expert_gate, "w_expert_up": w_expert_up, "w_expert_down": w_expert_down}


def rms_scale(values, gain):
    wide = values.astype(jnp.float32)
    return wide * lax.rsqrt(lax.optimization_barrier(jnp.mean(wide * wide, axis=-1, keepdims=True)) + 1e-06) * gain

def halves_sum(hidden, down, rows):
    split_hidden = hidden.reshape(rows, N_TP, -1).astype(jnp.float32)
    split_down = down.reshape(N_TP, -1, D).astype(jnp.float32)
    parts = jnp.einsum('rnf,nfd->nrd', split_hidden, split_down).astype(jnp.bfloat16)
    return lax.optimization_barrier(jnp.sum(parts.astype(jnp.float32), axis=0))

def reference(tokens, lengths, attn_gain, w_query, w_key, w_value, head_bias, key_cache, value_cache, w_attn_out, ffn_gain, w_router, routes, w_dense_gate, w_dense_up, w_dense_down, dense_mix, w_expert_gate, w_expert_up, w_expert_down):
    normed = rms_scale(tokens, attn_gain).astype(jnp.bfloat16)
    queries = jnp.dot(normed, w_query, preferred_element_type=jnp.float32).astype(jnp.bfloat16)
    new_keys = jnp.dot(normed, w_key, preferred_element_type=jnp.float32).astype(jnp.bfloat16)
    new_values = jnp.dot(normed, w_value, preferred_element_type=jnp.float32).astype(jnp.bfloat16)
    group_size = HEADS // KV_HEADS
    block_total = TOKENS // SEQ_DEV
    grouped = queries.reshape(block_total, SEQ_DEV, KV_HEADS, group_size, HEAD)
    key_blocks = key_cache.reshape(block_total, SEQ_DEV, KV_HEADS, HEAD, CACHE)
    value_blocks = value_cache.reshape(block_total, SEQ_DEV, KV_HEADS, HEAD, CACHE)
    length_blocks = lengths.reshape(block_total, SEQ_DEV)
    head_shift = head_bias.reshape(1, KV_HEADS, group_size, 1)

    def attend(inputs):
        block_queries, block_keys, block_values, block_lengths = inputs
        scores = jnp.einsum('skgd,skdc->skgc', block_queries.astype(jnp.float32), block_keys.astype(jnp.float32)) * HEAD ** (-0.5) + head_shift
        visible = (jnp.arange(CACHE, dtype=jnp.int32)[None, :] < block_lengths[:, None])[:, None, None, :]
        log_keep = jnp.where(visible, jax.nn.log_sigmoid(-scores), 0.0)
        log_after = lax.cumsum(log_keep, axis=3, reverse=True) - log_keep
        weights = jnp.where(visible, jnp.exp(jax.nn.log_sigmoid(scores) + log_after), 0.0).astype(jnp.bfloat16)
        mixed = jnp.einsum('skgc,skdc->skgd', weights.astype(jnp.float32), block_values.astype(jnp.float32))
        return mixed.reshape(SEQ_DEV, HEADS * HEAD).astype(jnp.bfloat16)
    heads_out = lax.map(attend, (grouped, key_blocks, value_blocks, length_blocks)).reshape(TOKENS, HEADS * HEAD)
    attn = halves_sum(heads_out, w_attn_out, TOKENS)
    residual = (tokens.astype(jnp.float32) + attn).astype(jnp.bfloat16)
    normed2 = rms_scale(residual, ffn_gain).astype(jnp.bfloat16)
    probs = jax.nn.sigmoid(jnp.dot(normed2, w_router, preferred_element_type=jnp.float32))
    hits = routes[:, :, None] == jnp.arange(EXPERTS, dtype=jnp.int32)[None, None, :]
    picked = lax.optimization_barrier(jnp.sum(jnp.where(hits, probs[:, None, :], 0.0), axis=-1))
    gates = picked / lax.optimization_barrier(jnp.sum(picked, axis=-1, keepdims=True)) * 2.5
    flat_routes = routes.reshape(-1)
    route_total = TOKENS * TOP_K
    bound = N_EP * CAP
    padded_inputs = jnp.concatenate([normed2, jnp.zeros((1, D), jnp.bfloat16)], axis=0)

    def expert_pass(inputs):
        expert_id, gate_w, up_w, down_w = inputs
        chosen = jnp.nonzero(flat_routes == expert_id, size=bound, fill_value=route_total)[0].astype(jnp.int32)
        rows_in = padded_inputs[chosen // TOP_K]
        gate_rows = jnp.dot(rows_in, gate_w, preferred_element_type=jnp.float32)
        up_rows = jnp.dot(rows_in, up_w, preferred_element_type=jnp.float32)
        hidden = (jax.nn.silu(gate_rows) * up_rows).astype(jnp.bfloat16)
        return (halves_sum(hidden, down_w, bound).astype(jnp.bfloat16), chosen)
    expert_rows, chosen_all = lax.map(expert_pass, (jnp.arange(EXPERTS, dtype=jnp.int32), w_expert_gate, w_expert_up, w_expert_down))
    route_rows = jnp.zeros((route_total + 1, D), jnp.bfloat16).at[chosen_all.reshape(-1)].set(expert_rows.reshape(-1, D))[:route_total]
    routed = lax.optimization_barrier(jnp.sum(gates[:, :, None] * route_rows.reshape(TOKENS, TOP_K, D).astype(jnp.float32), axis=1))
    dense_gate_rows = jnp.dot(normed2, w_dense_gate, preferred_element_type=jnp.float32)
    dense_up_rows = jnp.dot(normed2, w_dense_up, preferred_element_type=jnp.float32)
    dense_hidden = (jax.nn.silu(dense_gate_rows) * dense_up_rows).astype(jnp.bfloat16)
    dense = halves_sum(dense_hidden, w_dense_down, TOKENS)
    mix_gate = jax.nn.sigmoid(lax.optimization_barrier(jnp.sum(normed2.astype(jnp.float32) * dense_mix, axis=-1)))
    layer_out = (residual.astype(jnp.float32) + mix_gate[:, None] * dense + routed).astype(jnp.bfloat16)
    return (layer_out, new_keys, new_values)
```

```python
import functools

import jax
import jax.numpy as jnp
from jax import lax
from jax.experimental import pallas as pl
from jax.experimental.pallas import tpu as pltpu
from jax.sharding import PartitionSpec as P


def rms_scale(values, gain):
    wide = values.astype(jnp.float32)
    return wide * lax.rsqrt(jnp.mean(wide * wide, axis=-1, keepdims=True) + 1e-06) * gain


def stick_read(queries, lengths, head_bias, key_cache, value_cache):
    seq_count, local_kv, head_dim, cache_len = key_cache.shape
    group_size = head_bias.shape[0] // local_kv
    grouped = queries.reshape(seq_count, local_kv, group_size, head_dim)
    head_shift = head_bias.reshape(1, local_kv, group_size, 1)
    span_len = min(512, cache_len)
    block_count = (jnp.max(lengths) + span_len - 1) // span_len
    span_index = lax.iota(jnp.int32, span_len)
    after_mask = (span_index[:, None] > span_index[None, :]).astype(jnp.float32)

    def visit(visit_index, carry):
        totals, log_later = carry
        first = (block_count - 1 - visit_index) * span_len
        key_block = lax.dynamic_slice_in_dim(key_cache, first, span_len, 3)
        value_block = lax.dynamic_slice_in_dim(value_cache, first, span_len, 3)
        scores = (
            jnp.einsum("skgd,skdc->skgc", grouped, key_block, preferred_element_type=jnp.float32)
            * head_dim ** (-0.5)
            + head_shift
        )
        positions = first + span_index
        visible = (positions[None, :] < lengths[:, None])[:, None, None, :]
        log_keep = jnp.where(visible, jax.nn.log_sigmoid(-scores), 0.0)
        log_after = (
            jnp.einsum("skgj,jc->skgc", log_keep, after_mask, precision=lax.Precision.HIGHEST)
            + log_later[..., None]
        )
        weights = jnp.where(visible, jnp.exp(jax.nn.log_sigmoid(scores) + log_after), 0.0).astype(
            jnp.bfloat16
        )
        totals = totals + jnp.einsum(
            "skgc,skdc->skgd", weights, value_block, preferred_element_type=jnp.float32
        )
        return (totals, log_later + jnp.sum(log_keep, axis=3))

    start_totals = jnp.zeros((seq_count, local_kv, group_size, head_dim), jnp.float32)
    start_later = jnp.zeros((seq_count, local_kv, group_size), jnp.float32)
    totals, unused_later = lax.fori_loop(0, block_count, visit, (start_totals, start_later))
    return totals.reshape(seq_count, -1).astype(jnp.bfloat16)


MESH = pl.DeviceIdType.MESH


def after_attention(
    n,
    width,
    heads_ref,
    tokens_ref,
    gain_ref,
    router_ref,
    routes_ref,
    mix_ref,
    paired_ref,
    down_ref,
    w_out_hbm,
    w_gate_hbm,
    w_up_hbm,
    w_down_hbm,
    out_ref,
    w_out,
    w_gate,
    w_up,
    w_down,
    load_sem,
    attn_mine,
    attn_peer,
    res_ref,
    norm_all,
    part_send,
    part_recv,
    hidden_ref,
    dense_all,
    cols_send,
    cols_recv,
    other_ref,
    mine_ref,
    peer_ref,
    back_send,
    back_recv,
    pair_sems,
    norm_sems,
    pass_sems,
    part_sems,
    dense_sems,
    cols_send_sem,
    cols_recv_sem,
    back_sems,
):
    me = lax.axis_index("ep")
    core = lax.axis_index("tp")
    peer = 1 - core
    rows, model = tokens_ref.shape
    half = model // 2
    window = paired_ref.shape[0]
    first = (me * width) // window * window
    owner = first // half
    lane = pl.multiple_of(first % half, window)
    f32 = jnp.float32

    def remote(source, target, send_sem, recv_sem, ep, tp):
        return pltpu.make_async_remote_copy(
            src_ref=source,
            dst_ref=target,
            send_sem=send_sem,
            recv_sem=recv_sem,
            device_id=(ep, tp),
            device_id_type=MESH,
        )

    loads = [
        pltpu.make_async_copy(source, target, load_sem.at[i])
        for i, (source, target) in enumerate(
            ((w_out_hbm, w_out), (w_gate_hbm, w_gate), (w_up_hbm, w_up), (w_down_hbm, w_down))
        )
    ]
    for load in loads:
        load.start()

    barrier = pltpu.get_barrier_semaphore()

    def greet(k, carry):
        other = lax.rem(me + k, n)
        pl.semaphore_signal(barrier, inc=1, device_id=(other, core), device_id_type=MESH)
        pl.semaphore_signal(barrier, inc=1, device_id=(other, peer), device_id_type=MESH)
        return carry

    lax.fori_loop(1, n, greet, 0)
    pl.semaphore_signal(barrier, inc=1, device_id=(me, peer), device_id_type=MESH)

    loads[0].wait()
    attn_mine[...] = jnp.dot(heads_ref[...], w_out[...], preferred_element_type=f32).astype(
        jnp.bfloat16
    )
    pl.semaphore_wait(barrier, 2 * n - 1)

    swap = remote(attn_mine, attn_peer, pair_sems.at[0], pair_sems.at[1], me, peer)
    swap.start()
    swap.wait()
    attn = attn_mine[...].astype(f32) + attn_peer[...].astype(f32)
    residual = (tokens_ref[...].astype(f32) + attn).astype(jnp.bfloat16)
    res_ref[...] = residual
    wide = residual.astype(f32)
    normed = (
        wide * lax.rsqrt(jnp.mean(wide * wide, axis=-1, keepdims=True) + 1e-06) * gain_ref[...]
    ).astype(jnp.bfloat16)
    norm_all[0, me] = normed[:, :half]
    norm_all[1, me] = normed[:, half:]

    def norm_copy(j, other):
        return remote(
            norm_all.at[core, j],
            norm_all.at[core, j],
            norm_sems.at[0, other],
            norm_sems.at[1, j],
            other,
            core,
        )

    def pass_copy(j, which):
        return remote(
            norm_all.at[which, j],
            norm_all.at[which, j],
            pass_sems.at[0, j],
            pass_sems.at[1, j],
            me,
            peer,
        )

    def send_norm(k, carry):
        norm_copy(me, lax.rem(me + k, n)).start()
        return carry

    lax.fori_loop(1, n, send_norm, 0)

    probs = jax.nn.sigmoid(jnp.dot(normed, router_ref[...], preferred_element_type=f32))
    expert_total = probs.shape[1]
    expert_index = lax.broadcasted_iota(jnp.int32, (rows, expert_total), 1)
    hits = jnp.zeros((rows, expert_total), f32)
    for k in range(routes_ref.shape[1]):
        hits = jnp.where(routes_ref[:, k : k + 1] == expert_index, 1.0, hits)
    picked = jnp.where(hits > 0.0, probs, 0.0)
    gates = picked / jnp.sum(picked, axis=-1, keepdims=True) * 2.5
    mix_gate = jax.nn.sigmoid(
        jnp.sum(normed.astype(f32) * mix_ref[...], axis=-1, keepdims=True)
    )

    def take_norm(k, carry):
        j = lax.rem(me + n - k, n)
        norm_copy(j, me).wait_recv()
        pass_copy(j, core).start()
        return carry

    lax.fori_loop(1, n, take_norm, 0)

    def take_pass(k, carry):
        pass_copy(lax.rem(me + n - k, n), peer).wait_recv()
        return carry

    lax.fori_loop(1, n, take_pass, 0)

    def part_copy(j, other):
        return remote(
            part_send.at[other],
            part_recv.at[j],
            part_sems.at[0, other],
            part_sems.at[1, j],
            other,
            core,
        )

    def back_copy(j, other):
        return remote(
            back_send.at[other],
            back_recv.at[j],
            back_sems.at[0, other],
            back_sems.at[1, j],
            other,
            core,
        )

    def dense_copy(j, other):
        return remote(
            dense_all.at[j],
            dense_all.at[j],
            dense_sems.at[0, other],
            dense_sems.at[1, j],
            other,
            core,
        )

    group = min(n, 16)
    groups = n // group
    block = group * rows

    def dense_first(c, carry):
        base = c * group
        features = norm_all[owner, pl.ds(base, group), :, pl.ds(lane, window)]
        value = jnp.dot(
            features.reshape(block, window), paired_ref[...], preferred_element_type=f32
        )
        part_send[pl.ds(base, group)] = value.astype(jnp.bfloat16).reshape(group, rows, -1)
        return carry

    lax.fori_loop(0, groups, dense_first, 0)

    def send_part(k, carry):
        part_copy(me, lax.rem(me + k, n)).start()
        return carry

    lax.fori_loop(1, n, send_part, 0)

    loads[1].wait()
    loads[2].wait()

    def expert_first(c, carry):
        base = c * group
        low = norm_all[0, pl.ds(base, group)].reshape(block, half)
        high = norm_all[1, pl.ds(base, group)].reshape(block, half)
        gate_rows = jnp.dot(low, w_gate[:half], preferred_element_type=f32) + jnp.dot(
            high, w_gate[half:], preferred_element_type=f32
        )
        up_rows = jnp.dot(low, w_up[:half], preferred_element_type=f32) + jnp.dot(
            high, w_up[half:], preferred_element_type=f32
        )
        hidden_ref[pl.ds(c, 1)] = (jax.nn.silu(gate_rows) * up_rows).astype(jnp.bfloat16)[None]
        return carry

    lax.fori_loop(0, groups, expert_first, 0)

    def take_part(k, total):
        j = lax.rem(me + n - k, n)
        part_copy(j, me).wait_recv()
        return total + part_recv[j].astype(f32)

    paired = lax.fori_loop(1, n, take_part, part_send[me].astype(f32))
    hidden_cols = paired.shape[1] // 2
    dense_all[me] = (jax.nn.silu(paired[:, :hidden_cols]) * paired[:, hidden_cols:]).astype(
        jnp.bfloat16
    )

    def send_dense(k, carry):
        dense_copy(me, lax.rem(me + k, n)).start()
        return carry

    lax.fori_loop(1, n, send_dense, 0)

    loads[3].wait()
    far = pl.ds(pl.multiple_of(peer * half, half), half)
    near = pl.ds(pl.multiple_of(core * half, half), half)

    def expert_far(c, carry):
        value = jnp.dot(hidden_ref[c], w_down[:, far], preferred_element_type=f32)
        other_ref[pl.ds(c * group, group)] = value.astype(jnp.bfloat16).reshape(group, rows, half)
        return carry

    lax.fori_loop(0, groups, expert_far, 0)
    trade = remote(other_ref, peer_ref, pair_sems.at[2], pair_sems.at[3], me, peer)
    trade.start()

    def expert_near(c, carry):
        value = jnp.dot(hidden_ref[c], w_down[:, near], preferred_element_type=f32)
        mine_ref[pl.ds(c * group, group)] = value.astype(jnp.bfloat16).reshape(group, rows, half)
        return carry

    lax.fori_loop(0, groups, expert_near, 0)
    trade.wait()

    def send_back(k, carry):
        other = lax.rem(me + k, n)
        total = mine_ref[other].astype(f32) + peer_ref[other].astype(f32)
        back_send[other] = total.astype(jnp.bfloat16)

        @pl.when(k > 0)
        def _():
            back_copy(me, other).start()

        return carry

    lax.fori_loop(0, n, send_back, 0)

    def take_dense(k, carry):
        dense_copy(lax.rem(me + n - k, n), me).wait_recv()
        return carry

    lax.fori_loop(1, n, take_dense, 0)

    def dense_second(c, carry):
        base = c * group
        value = jnp.dot(
            dense_all[pl.ds(base, group)].reshape(block, hidden_cols),
            down_ref[...],
            preferred_element_type=f32,
        )
        cols_send[pl.ds(base, group)] = value.astype(jnp.bfloat16).reshape(group, rows, window)
        return carry

    lax.fori_loop(0, groups, dense_second, 0)

    def cols_copy(from_core, j, other, target):
        return remote(
            cols_send.at[other],
            cols_recv.at[from_core, j],
            cols_send_sem.at[other],
            cols_recv_sem.at[from_core, j],
            other,
            target,
        )

    def send_cols(k, carry):
        cols_copy(core, me, lax.rem(me + k, n), owner).start()
        return carry

    lax.fori_loop(1, n, send_cols, 0)

    @pl.when(owner == core)
    def _():
        cols_recv[core, me] = cols_send[me]

    @pl.when(owner != core)
    def _():
        cols_copy(core, me, me, peer).start()

    def take_cols(k, carry):
        j = core * (n // 2) + k

        @pl.when(j != me)
        def _():
            cols_copy(core, j, me, core).wait_recv()

        cols_copy(peer, j, me, core).wait_recv()
        return carry

    lax.fori_loop(0, n // 2, take_cols, 0)
    per_window = window // width
    dense_parts = []
    for q in range(half // window):
        total = jnp.zeros((rows, window), f32)
        for r in range(per_window):
            j = core * (n // 2) + q * per_window + r
            total = total + cols_recv[0, j].astype(f32) + cols_recv[1, j].astype(f32)
        dense_parts.append(total)
    dense = jnp.concatenate(dense_parts, axis=1)
    total = res_ref[:, near].astype(f32) + mix_gate * dense

    def take_back(k, total):
        j = lax.rem(me + n - k, n)

        @pl.when(k > 0)
        def _():
            back_copy(j, me).wait_recv()

        @pl.when(k == 0)
        def _():
            back_recv[me] = back_send[me]

        gate = jnp.sum(jnp.where(expert_index == j, gates, 0.0), axis=-1, keepdims=True)
        return total + gate * back_recv[j].astype(f32)

    out_ref[...] = lax.fori_loop(0, n, take_back, total).astype(jnp.bfloat16)

    def drain(k, carry):
        other = lax.rem(me + k, n)
        norm_copy(me, other).wait_send()
        pass_copy(other, core).wait_send()
        part_copy(me, other).wait_send()
        dense_copy(me, other).wait_send()
        cols_copy(core, me, other, owner).wait_send()
        back_copy(me, other).wait_send()
        return carry

    lax.fori_loop(1, n, drain, 0)

    @pl.when(owner != core)
    def _():
        cols_copy(core, me, me, peer).wait_send()


def shards(
    n,
    tokens,
    lengths,
    attn_gain,
    w_query,
    w_key,
    w_value,
    head_bias,
    key_cache,
    value_cache,
    w_attn_out,
    ffn_gain,
    w_router,
    routes,
    w_dense_gate,
    w_dense_up,
    w_dense_down,
    dense_mix,
    w_expert_gate,
    w_expert_up,
    w_expert_down,
):
    rows, model = tokens.shape
    half = model // 2
    normed = rms_scale(tokens, attn_gain).astype(jnp.bfloat16)
    new_keys = jnp.dot(normed, w_key, preferred_element_type=jnp.float32).astype(jnp.bfloat16)
    new_values = jnp.dot(normed, w_value, preferred_element_type=jnp.float32).astype(jnp.bfloat16)
    queries = jnp.dot(normed, w_query, preferred_element_type=jnp.float32).astype(jnp.bfloat16)
    heads_out = stick_read(queries, lengths, head_bias, key_cache, value_cache)

    width, hidden_cols = w_dense_gate.shape
    window = max(width, 128)
    paired = jnp.concatenate([w_dense_gate, w_dense_up], axis=1)
    down = w_dense_down
    if window != width:
        shift = (lax.axis_index("ep") * width) % window
        paired = lax.dynamic_update_slice(
            jnp.zeros((window, paired.shape[1]), paired.dtype), paired, (shift, 0)
        )
        down = lax.dynamic_update_slice(
            jnp.zeros((hidden_cols, window), down.dtype), down, (0, shift)
        )
    w_gate, w_up, w_down = w_expert_gate[0], w_expert_up[0], w_expert_down[0]
    expert_hidden = w_gate.shape[1]
    bf16 = jnp.bfloat16
    block = min(n, 16) * rows
    vmem = pl.BlockSpec(memory_space=pltpu.VMEM)
    anywhere = pl.BlockSpec(memory_space=pl.ANY)
    dma = pltpu.SemaphoreType.DMA
    layer_out = pl.pallas_call(
        functools.partial(after_attention, n, width),
        out_shape=jax.ShapeDtypeStruct((rows, half), bf16),
        in_specs=[vmem] * 8 + [anywhere] * 4,
        out_specs=vmem,
        scratch_shapes=[
            pltpu.VMEM(w_attn_out.shape, bf16),
            pltpu.VMEM(w_gate.shape, bf16),
            pltpu.VMEM(w_up.shape, bf16),
            pltpu.VMEM(w_down.shape, bf16),
            dma((4,)),
            pltpu.VMEM((rows, model), bf16),
            pltpu.VMEM((rows, model), bf16),
            pltpu.VMEM((rows, model), bf16),
            pltpu.VMEM((2, n, rows, half), bf16),
            pltpu.VMEM((n, rows, 2 * hidden_cols), bf16),
            pltpu.VMEM((n, rows, 2 * hidden_cols), bf16),
            pltpu.VMEM((n * rows // block, block, expert_hidden), bf16),
            pltpu.VMEM((n, rows, hidden_cols), bf16),
            pltpu.VMEM((n, rows, window), bf16),
            pltpu.VMEM((2, n, rows, window), bf16),
            pltpu.VMEM((n, rows, half), bf16),
            pltpu.VMEM((n, rows, half), bf16),
            pltpu.VMEM((n, rows, half), bf16),
            pltpu.VMEM((n, rows, half), bf16),
            pltpu.VMEM((n, rows, half), bf16),
            dma((4,)),
            dma((2, n)),
            dma((2, n)),
            dma((2, n)),
            dma((2, n)),
            dma((n,)),
            dma((2, n)),
            dma((2, n)),
        ],
        compiler_params=pltpu.CompilerParams(
            collective_id=0, has_side_effects=True, vmem_limit_bytes=48 * 1024 * 1024
        ),
        name="after_attention",
    )(
        heads_out,
        tokens,
        ffn_gain.reshape(1, model),
        w_router,
        routes,
        dense_mix.reshape(1, model),
        paired,
        down,
        w_attn_out,
        w_gate,
        w_up,
        w_down,
    )
    return (layer_out, new_keys, new_values)


def solution(mesh):
    return jax.shard_map(
        functools.partial(shards, mesh.shape["ep"]),
        mesh=mesh,
        in_specs=(
            P("ep", None),
            P("ep"),
            P(),
            P(None, "tp"),
            P(None, "tp"),
            P(None, "tp"),
            P("tp"),
            P("ep", "tp", None, None),
            P("ep", "tp", None, None),
            P("tp", None),
            P(),
            P(),
            P("ep", None),
            P("ep", "tp"),
            P("ep", "tp"),
            P("tp", "ep"),
            P(),
            P("ep", None, "tp"),
            P("ep", None, "tp"),
            P("ep", "tp", None),
        ),
        out_specs=(P("ep", "tp"), P("ep", "tp"), P("ep", "tp")),
        check_vma=False,
    )
```

```python
import functools

import jax
import jax.numpy as jnp
from jax import lax
from jax.experimental import pallas as pl
from jax.experimental.pallas import tpu as pltpu
from jax.sharding import PartitionSpec as P

MESH = pl.DeviceIdType.MESH


def whole_layer(
    n,
    group_size,
    tokens_ref,
    attn_gain_ref,
    limits_ref,
    bias_ref,
    w_key_ref,
    w_value_ref,
    gain_ref,
    router_ref,
    routes_ref,
    mix_ref,
    paired_ref,
    down_ref,
    w_query_hbm,
    w_out_hbm,
    w_gate_hbm,
    w_up_hbm,
    w_down_hbm,
    keys_hbm,
    values_hbm,
    out_ref,
    new_keys_ref,
    new_values_ref,
    w_query,
    w_out,
    w_gate,
    w_up,
    w_down,
    keys,
    values,
    load_sem,
    keys_sem,
    values_sem,
    query_ref,
    score_ref,
    read_ref,
    normed_ref,
    paired_all,
    down_all,
    attn_mine,
    attn_peer,
    res_ref,
    norm_all,
    part_send,
    part_recv,
    hidden_ref,
    dense_all,
    cols_send,
    cols_recv,
    other_ref,
    mine_ref,
    peer_ref,
    back_send,
    back_recv,
    pair_sems,
    paired_sems,
    down_sems,
    norm_sems,
    pass_sems,
    part_sems,
    dense_sems,
    cols_send_sem,
    cols_recv_sem,
    back_sems,
):
    me = lax.axis_index("ep")
    core = lax.axis_index("tp")
    peer = 1 - core
    rows, model = tokens_ref.shape
    half = model // 2
    width = paired_ref.shape[0]
    window = width * group_size
    place = me % group_size
    team = me // group_size
    teams = n // group_size
    first = team * window
    owner = first // half
    lane = pl.multiple_of(first % half, window)
    f32 = jnp.float32
    local_heads = bias_ref.shape[0]
    head_dim, cache_len = keys_hbm.shape[1:]
    span = 4

    def remote(source, target, send_sem, recv_sem, ep, tp):
        return pltpu.make_async_remote_copy(
            src_ref=source,
            dst_ref=target,
            send_sem=send_sem,
            recv_sem=recv_sem,
            device_id=(ep, tp),
            device_id_type=MESH,
        )

    pairs = (
        (w_query_hbm, w_query),
        (w_gate_hbm, w_gate),
        (w_up_hbm, w_up),
        (w_down_hbm, w_down),
        (w_out_hbm, w_out),
    )
    loads = [
        pltpu.make_async_copy(source, target, load_sem.at[i])
        for i, (source, target) in enumerate(pairs)
    ]

    def keys_load(c):
        block = pl.ds(c * span, span)
        return pltpu.make_async_copy(keys_hbm.at[block], keys.at[block], keys_sem.at[c])

    def values_load(c):
        block = pl.ds(c * span, span)
        return pltpu.make_async_copy(values_hbm.at[block], values.at[block], values_sem.at[c])

    loads[0].start()
    for c in range(rows // span):
        keys_load(c).start()
        values_load(c).start()
    for load in (loads[4], loads[1], loads[2], loads[3]):
        load.start()

    barrier = pltpu.get_barrier_semaphore()

    def greet(k, carry):
        other = lax.rem(me + k, n)
        pl.semaphore_signal(barrier, inc=1, device_id=(other, core), device_id_type=MESH)
        pl.semaphore_signal(barrier, inc=1, device_id=(other, peer), device_id_type=MESH)
        return carry

    lax.fori_loop(1, n, greet, 0)
    pl.semaphore_signal(barrier, inc=1, device_id=(me, peer), device_id_type=MESH)

    start = tokens_ref[...].astype(f32)
    normed_ref[...] = (
        start
        * lax.rsqrt(jnp.mean(start * start, axis=-1, keepdims=True) + 1e-06)
        * attn_gain_ref[...]
    ).astype(jnp.bfloat16)
    loads[0].wait()
    queries = jnp.dot(normed_ref[...], w_query[...], preferred_element_type=f32)
    queries = queries.astype(jnp.bfloat16).astype(f32)
    for h in range(local_heads):
        query_ref[:, h, :] = queries[:, h * head_dim : (h + 1) * head_dim]
    pl.semaphore_wait(barrier, 2 * n - 1)

    def team_copy(source, gathered, sems, origin, other):
        return remote(
            source,
            gathered.at[origin],
            sems.at[0, other],
            sems.at[1, origin],
            team * group_size + other,
            core,
        )

    def send_weights(k, carry):
        other = lax.rem(place + k, group_size)
        team_copy(paired_ref, paired_all, paired_sems, place, other).start()
        team_copy(down_ref, down_all, down_sems, place, other).start()
        return carry

    lax.fori_loop(1, group_size, send_weights, 0)
    paired_all[place] = paired_ref[...]
    down_all[place] = down_ref[...]

    block_len = min(256, cache_len)
    after_mask = (
        lax.broadcasted_iota(jnp.int32, (block_len, block_len), 0)
        > lax.broadcasted_iota(jnp.int32, (block_len, block_len), 1)
    ).astype(jnp.bfloat16)
    position = lax.broadcasted_iota(jnp.int32, (span * local_heads, block_len), 1)

    def attend(c, carry):
        keys_load(c).wait()
        lines = span * local_heads
        for i in range(span):
            s = c * span + i
            score_ref[s] = (
                jnp.dot(query_ref[s].astype(jnp.bfloat16), keys[s], preferred_element_type=f32)
                * head_dim ** (-0.5)
                + bias_ref[...]
            )
        limits = limits_ref[pl.ds(c * lines, lines)]
        later = jnp.zeros((lines, 1), f32)
        for first_pos in range(cache_len - block_len, -1, -block_len):
            columns = slice(first_pos, first_pos + block_len)
            scores = score_ref[pl.ds(c * span, span), :, columns].reshape(lines, block_len)
            visible = position + first_pos < limits
            keep = -(jnp.maximum(scores, 0.0) + jnp.log1p(jnp.exp(-jnp.abs(scores))))
            log_take = scores + keep
            keep = jnp.where(visible, keep, 0.0)
            top = keep.astype(jnp.bfloat16)
            rest = keep - top.astype(f32)
            middle = rest.astype(jnp.bfloat16)
            low = (rest - middle.astype(f32)).astype(jnp.bfloat16)
            sums = jnp.dot(
                jnp.concatenate([top, middle, low], axis=0),
                after_mask,
                preferred_element_type=f32,
            )
            after = sums[:lines] + sums[lines : 2 * lines] + sums[2 * lines :] + later
            later = later + jnp.sum(keep, axis=-1, keepdims=True)
            stick = jnp.where(visible, jnp.exp(log_take + after), 0.0)
            score_ref[pl.ds(c * span, span), :, columns] = stick.reshape(
                span, local_heads, block_len
            )
        values_load(c).wait()
        for i in range(span):
            s = c * span + i
            read_ref[s] = lax.dot_general(
                score_ref[s].astype(jnp.bfloat16),
                values[s],
                (((1,), (1,)), ((), ())),
                preferred_element_type=f32,
            )
        return carry

    lax.fori_loop(0, rows // span, attend, 0)
    heads_out = jnp.concatenate(
        [read_ref[:, h, :] for h in range(local_heads)], axis=1
    ).astype(jnp.bfloat16)
    loads[4].wait()
    attn_mine[...] = jnp.dot(heads_out, w_out[...], preferred_element_type=f32).astype(
        jnp.bfloat16
    )

    swap = remote(attn_mine, attn_peer, pair_sems.at[0], pair_sems.at[1], me, peer)
    swap.start()
    swap.wait()
    attn = attn_mine[...].astype(f32) + attn_peer[...].astype(f32)
    residual = (tokens_ref[...].astype(f32) + attn).astype(jnp.bfloat16)
    res_ref[...] = residual
    wide = residual.astype(f32)
    normed = (
        wide * lax.rsqrt(jnp.mean(wide * wide, axis=-1, keepdims=True) + 1e-06) * gain_ref[...]
    ).astype(jnp.bfloat16)
    norm_all[0, me] = normed[:, :half]
    norm_all[1, me] = normed[:, half:]

    def norm_copy(j, other):
        return remote(
            norm_all.at[core, j],
            norm_all.at[core, j],
            norm_sems.at[0, other],
            norm_sems.at[1, j],
            other,
            core,
        )

    def pass_copy(j, which):
        return remote(
            norm_all.at[which, j],
            norm_all.at[which, j],
            pass_sems.at[0, j],
            pass_sems.at[1, j],
            me,
            peer,
        )

    def send_norm(k, carry):
        norm_copy(me, lax.rem(me + k, n)).start()
        return carry

    lax.fori_loop(1, n, send_norm, 0)

    probs = jax.nn.sigmoid(jnp.dot(normed, router_ref[...], preferred_element_type=f32))
    expert_total = probs.shape[1]
    expert_index = lax.broadcasted_iota(jnp.int32, (rows, expert_total), 1)
    hits = jnp.zeros((rows, expert_total), f32)
    for k in range(routes_ref.shape[1]):
        hits = jnp.where(routes_ref[:, k : k + 1] == expert_index, 1.0, hits)
    picked = jnp.where(hits > 0.0, probs, 0.0)
    gates = picked / jnp.sum(picked, axis=-1, keepdims=True) * 2.5
    mix_gate = jax.nn.sigmoid(
        jnp.sum(normed.astype(f32) * mix_ref[...], axis=-1, keepdims=True)
    )

    for weight, target in ((w_key_ref, new_keys_ref), (w_value_ref, new_values_ref)):
        target[...] = jnp.dot(normed_ref[...], weight[...], preferred_element_type=f32).astype(
            jnp.bfloat16
        )

    def take_norm(k, carry):
        j = lax.rem(me + n - k, n)
        norm_copy(j, me).wait_recv()
        pass_copy(j, core).start()
        return carry

    lax.fori_loop(1, n, take_norm, 0)

    def take_pass(k, carry):
        pass_copy(lax.rem(me + n - k, n), peer).wait_recv()
        return carry

    lax.fori_loop(1, n, take_pass, 0)

    def part_copy(m, other):
        return remote(
            part_send.at[other],
            part_recv.at[m],
            part_sems.at[0, other],
            part_sems.at[1, m],
            other * group_size + place,
            core,
        )

    def back_copy(j, other):
        return remote(
            back_send.at[other],
            back_recv.at[j],
            back_sems.at[0, other],
            back_sems.at[1, j],
            other,
            core,
        )

    def dense_copy(m, other):
        return remote(
            dense_all.at[m],
            dense_all.at[m],
            dense_sems.at[0, other],
            dense_sems.at[1, m],
            other * group_size + place,
            core,
        )

    group = min(n, 16)
    groups = n // group
    block = group * rows

    def take_weights(k, carry):
        other = lax.rem(place + k, group_size)
        team_copy(paired_ref, paired_all, paired_sems, other, place).wait_recv()
        team_copy(down_ref, down_all, down_sems, other, place).wait_recv()
        return carry

    lax.fori_loop(1, group_size, take_weights, 0)
    features = jnp.concatenate(
        [norm_all[owner, m * group_size + place, :, pl.ds(lane, window)] for m in range(teams)],
        axis=0,
    )
    part_send[...] = (
        jnp.dot(
            features, paired_all[...].reshape(window, -1), preferred_element_type=f32
        )
        .astype(jnp.bfloat16)
        .reshape(part_send.shape)
    )

    def send_part(k, carry):
        part_copy(team, lax.rem(team + k, teams)).start()
        return carry

    lax.fori_loop(1, teams, send_part, 0)

    loads[1].wait()
    loads[2].wait()

    def expert_first(c, carry):
        base = c * group
        low = norm_all[0, pl.ds(base, group)].reshape(block, half)
        high = norm_all[1, pl.ds(base, group)].reshape(block, half)
        gate_rows = jnp.dot(low, w_gate[:half], preferred_element_type=f32) + jnp.dot(
            high, w_gate[half:], preferred_element_type=f32
        )
        up_rows = jnp.dot(low, w_up[:half], preferred_element_type=f32) + jnp.dot(
            high, w_up[half:], preferred_element_type=f32
        )
        hidden_ref[pl.ds(c, 1)] = (jax.nn.silu(gate_rows) * up_rows).astype(jnp.bfloat16)[None]
        return carry

    lax.fori_loop(0, groups, expert_first, 0)

    def take_part(k, total):
        m = lax.rem(team + teams - k, teams)
        part_copy(m, team).wait_recv()
        return total + part_recv[m].astype(f32)

    paired = lax.fori_loop(1, teams, take_part, part_send[team].astype(f32))
    hidden_cols = paired.shape[1] // 2
    dense_all[team] = (jax.nn.silu(paired[:, :hidden_cols]) * paired[:, hidden_cols:]).astype(
        jnp.bfloat16
    )

    def send_dense(k, carry):
        dense_copy(team, lax.rem(team + k, teams)).start()
        return carry

    lax.fori_loop(1, teams, send_dense, 0)

    loads[3].wait()
    far = pl.ds(pl.multiple_of(peer * half, half), half)
    near = pl.ds(pl.multiple_of(core * half, half), half)

    def expert_far(c, carry):
        value = jnp.dot(hidden_ref[c], w_down[:, far], preferred_element_type=f32)
        other_ref[pl.ds(c * group, group)] = value.astype(jnp.bfloat16).reshape(group, rows, half)
        return carry

    lax.fori_loop(0, groups, expert_far, 0)
    trade = remote(other_ref, peer_ref, pair_sems.at[2], pair_sems.at[3], me, peer)
    trade.start()

    def expert_near(c, carry):
        value = jnp.dot(hidden_ref[c], w_down[:, near], preferred_element_type=f32)
        mine_ref[pl.ds(c * group, group)] = value.astype(jnp.bfloat16).reshape(group, rows, half)
        return carry

    lax.fori_loop(0, groups, expert_near, 0)
    trade.wait()

    def send_back(k, carry):
        other = lax.rem(me + k, n)
        total = mine_ref[other].astype(f32) + peer_ref[other].astype(f32)
        back_send[other] = total.astype(jnp.bfloat16)

        @pl.when(k > 0)
        def _():
            back_copy(me, other).start()

        return carry

    lax.fori_loop(0, n, send_back, 0)

    def take_dense(k, carry):
        dense_copy(lax.rem(team + teams - k, teams), team).wait_recv()
        return carry

    lax.fori_loop(1, teams, take_dense, 0)
    cols_send[...] = (
        lax.dot_general(
            dense_all[...].reshape(teams * rows, hidden_cols),
            down_all[...].reshape(window, hidden_cols),
            (((1,), (1,)), ((), ())),
            preferred_element_type=f32,
        )
        .astype(jnp.bfloat16)
        .reshape(cols_send.shape)
    )

    def cols_copy(from_core, m, other, target):
        return remote(
            cols_send.at[other],
            cols_recv.at[from_core, m],
            cols_send_sem.at[other],
            cols_recv_sem.at[from_core, m],
            other * group_size + place,
            target,
        )

    def send_cols(k, carry):
        cols_copy(core, team, lax.rem(team + k, teams), owner).start()
        return carry

    lax.fori_loop(1, teams, send_cols, 0)

    @pl.when(owner == core)
    def _():
        cols_recv[core, team] = cols_send[team]

    @pl.when(owner != core)
    def _():
        cols_copy(core, team, team, peer).start()

    side = teams // 2

    def take_cols(k, carry):
        m = core * side + k

        @pl.when(m != team)
        def _():
            cols_copy(core, m, team, core).wait_recv()

        cols_copy(peer, m, team, core).wait_recv()
        return carry

    lax.fori_loop(0, side, take_cols, 0)
    dense = jnp.concatenate(
        [
            cols_recv[0, core * side + q].astype(f32) + cols_recv[1, core * side + q].astype(f32)
            for q in range(side)
        ],
        axis=1,
    )
    total = res_ref[:, near].astype(f32) + mix_gate * dense

    def take_back(k, total):
        j = lax.rem(me + n - k, n)

        @pl.when(k > 0)
        def _():
            back_copy(j, me).wait_recv()

        @pl.when(k == 0)
        def _():
            back_recv[me] = back_send[me]

        gate = jnp.sum(jnp.where(expert_index == j, gates, 0.0), axis=-1, keepdims=True)
        return total + gate * back_recv[j].astype(f32)

    out_ref[...] = lax.fori_loop(0, n, take_back, total).astype(jnp.bfloat16)

    def drain(k, carry):
        other = lax.rem(me + k, n)
        norm_copy(me, other).wait_send()
        pass_copy(other, core).wait_send()
        back_copy(me, other).wait_send()
        return carry

    lax.fori_loop(1, n, drain, 0)

    def drain_team(k, carry):
        other = lax.rem(place + k, group_size)
        team_copy(paired_ref, paired_all, paired_sems, place, other).wait_send()
        team_copy(down_ref, down_all, down_sems, place, other).wait_send()
        return carry

    lax.fori_loop(1, group_size, drain_team, 0)

    def drain_dense(k, carry):
        other = lax.rem(team + k, teams)
        part_copy(team, other).wait_send()
        dense_copy(team, other).wait_send()
        cols_copy(core, team, other, owner).wait_send()
        return carry

    lax.fori_loop(1, teams, drain_dense, 0)

    @pl.when(owner != core)
    def _():
        cols_copy(core, team, team, peer).wait_send()


def shards(
    n,
    tokens,
    lengths,
    attn_gain,
    w_query,
    w_key,
    w_value,
    head_bias,
    key_cache,
    value_cache,
    w_attn_out,
    ffn_gain,
    w_router,
    routes,
    w_dense_gate,
    w_dense_up,
    w_dense_down,
    dense_mix,
    w_expert_gate,
    w_expert_up,
    w_expert_down,
):
    rows, model = tokens.shape
    half = model // 2
    width, hidden_cols = w_dense_gate.shape
    group_size = min(n, max(4, 128 // width))
    teams = n // group_size
    window = width * group_size
    paired = jnp.concatenate([w_dense_gate, w_dense_up], axis=1)
    down = w_dense_down.T
    seq_count, local_kv, head_dim, cache_len = key_cache.shape
    local_heads = head_bias.shape[0]
    keys = key_cache.reshape(seq_count, head_dim, cache_len)
    values = value_cache.reshape(seq_count, head_dim, cache_len)
    limits = jnp.repeat(lengths, local_heads).reshape(seq_count * local_heads, 1)
    w_gate, w_up, w_down = w_expert_gate[0], w_expert_up[0], w_expert_down[0]
    expert_hidden = w_gate.shape[1]
    bf16, f32 = jnp.bfloat16, jnp.float32
    block = min(n, 16) * rows
    vmem = pl.BlockSpec(memory_space=pltpu.VMEM)
    anywhere = pl.BlockSpec(memory_space=pl.ANY)
    dma = pltpu.SemaphoreType.DMA
    return pl.pallas_call(
        functools.partial(whole_layer, n, group_size),
        out_shape=(
            jax.ShapeDtypeStruct((rows, half), bf16),
            jax.ShapeDtypeStruct((rows, w_key.shape[1]), bf16),
            jax.ShapeDtypeStruct((rows, w_value.shape[1]), bf16),
        ),
        in_specs=[vmem] * 12 + [anywhere] * 7,
        out_specs=(vmem, vmem, vmem),
        scratch_shapes=[
            pltpu.VMEM(w_query.shape, bf16),
            pltpu.VMEM(w_attn_out.shape, bf16),
            pltpu.VMEM(w_gate.shape, bf16),
            pltpu.VMEM(w_up.shape, bf16),
            pltpu.VMEM(w_down.shape, bf16),
            pltpu.VMEM(keys.shape, bf16),
            pltpu.VMEM(values.shape, bf16),
            dma((5,)),
            dma((rows // 4,)),
            dma((rows // 4,)),
            pltpu.VMEM((rows, local_heads, head_dim), f32),
            pltpu.VMEM((rows, local_heads, cache_len), f32),
            pltpu.VMEM((rows, local_heads, head_dim), f32),
            pltpu.VMEM((rows, model), bf16),
            pltpu.VMEM((group_size, width, 2 * hidden_cols), bf16),
            pltpu.VMEM((group_size, width, hidden_cols), bf16),
            pltpu.VMEM((rows, model), bf16),
            pltpu.VMEM((rows, model), bf16),
            pltpu.VMEM((rows, model), bf16),
            pltpu.VMEM((2, n, rows, half), bf16),
            pltpu.VMEM((teams, rows, 2 * hidden_cols), bf16),
            pltpu.VMEM((teams, rows, 2 * hidden_cols), bf16),
            pltpu.VMEM((n * rows // block, block, expert_hidden), bf16),
            pltpu.VMEM((teams, rows, hidden_cols), bf16),
            pltpu.VMEM((teams, rows, window), bf16),
            pltpu.VMEM((2, teams, rows, window), bf16),
            pltpu.VMEM((n, rows, half), bf16),
            pltpu.VMEM((n, rows, half), bf16),
            pltpu.VMEM((n, rows, half), bf16),
            pltpu.VMEM((n, rows, half), bf16),
            pltpu.VMEM((n, rows, half), bf16),
            dma((4,)),
            dma((2, group_size)),
            dma((2, group_size)),
            dma((2, n)),
            dma((2, n)),
            dma((2, teams)),
            dma((2, teams)),
            dma((teams,)),
            dma((2, teams)),
            dma((2, n)),
        ],
        compiler_params=pltpu.CompilerParams(
            collective_id=0, has_side_effects=True, vmem_limit_bytes=60 * 1024 * 1024
        ),
        name="whole_layer",
    )(
        tokens,
        attn_gain.reshape(1, model),
        limits,
        head_bias.reshape(local_heads, 1),
        w_key,
        w_value,
        ffn_gain.reshape(1, model),
        w_router,
        routes,
        dense_mix.reshape(1, model),
        paired,
        down,
        w_query,
        w_attn_out,
        w_gate,
        w_up,
        w_down,
        keys,
        values,
    )


def solution(mesh):
    return jax.shard_map(
        functools.partial(shards, mesh.shape["ep"]),
        mesh=mesh,
        in_specs=(
            P("ep", None),
            P("ep"),
            P(),
            P(None, "tp"),
            P(None, "tp"),
            P(None, "tp"),
            P("tp"),
            P("ep", "tp", None, None),
            P("ep", "tp", None, None),
            P("tp", None),
            P(),
            P(),
            P("ep", None),
            P("ep", "tp"),
            P("ep", "tp"),
            P("tp", "ep"),
            P(),
            P("ep", None, "tp"),
            P("ep", None, "tp"),
            P("ep", "tp", None),
        ),
        out_specs=(P("ep", "tp"), P("ep", "tp"), P("ep", "tp")),
        check_vma=False,
    )
```

```python
import functools

import jax
import jax.numpy as jnp
from jax import lax
from jax.experimental import pallas as pl
from jax.experimental.pallas import tpu as pltpu
from jax.sharding import PartitionSpec as P

MESH = pl.DeviceIdType.MESH


def whole_layer(
    n,
    group_size,
    tokens_ref,
    attn_gain_ref,
    lengths_ref,
    bias_ref,
    w_key_ref,
    w_value_ref,
    gain_ref,
    router_ref,
    routes_ref,
    mix_ref,
    dense_gate_ref,
    dense_up_ref,
    down_ref,
    w_query_hbm,
    w_out_hbm,
    w_gate_hbm,
    w_up_hbm,
    w_down_hbm,
    keys_hbm,
    values_hbm,
    out_ref,
    new_keys_ref,
    new_values_ref,
    w_query,
    w_out,
    w_gate,
    w_up,
    w_down,
    keys,
    values,
    load_sem,
    keys_sem,
    values_sem,
    query_ref,
    score_ref,
    read_ref,
    normed_ref,
    dense_gate_all,
    dense_up_all,
    down_all,
    attn_mine,
    attn_peer,
    res_ref,
    norm_all,
    part_send,
    part_recv,
    hidden_ref,
    dense_all,
    cols_send,
    cols_recv,
    other_ref,
    mine_ref,
    peer_ref,
    back_send,
    back_recv,
    pair_sems,
    dense_gate_sems,
    dense_up_sems,
    down_sems,
    norm_sems,
    pass_sems,
    part_sems,
    dense_sems,
    cols_send_sem,
    cols_recv_sem,
    back_sems,
):
    me = lax.axis_index("ep")
    core = lax.axis_index("tp")
    peer = 1 - core
    rows, model = tokens_ref.shape
    half = model // 2
    width = dense_gate_ref.shape[0]
    window = width * group_size
    place = me % group_size
    team = me // group_size
    teams = n // group_size
    first = team * window
    owner = first // half
    lane = pl.multiple_of(first % half, window)
    f32 = jnp.float32
    local_heads = bias_ref.shape[1]
    head_dim, cache_len = keys_hbm.shape[1:]
    span = 4

    def remote(source, target, send_sem, recv_sem, ep, tp):
        return pltpu.make_async_remote_copy(
            src_ref=source,
            dst_ref=target,
            send_sem=send_sem,
            recv_sem=recv_sem,
            device_id=(ep, tp),
            device_id_type=MESH,
        )

    pairs = (
        (w_query_hbm, w_query),
        (w_gate_hbm, w_gate),
        (w_up_hbm, w_up),
        (w_down_hbm, w_down),
        (w_out_hbm, w_out),
    )
    loads = [
        pltpu.make_async_copy(source, target, load_sem.at[i])
        for i, (source, target) in enumerate(pairs)
    ]

    def keys_load(c):
        block = pl.ds(c * span, span)
        return pltpu.make_async_copy(keys_hbm.at[block], keys.at[block], keys_sem.at[c])

    def values_load(c):
        block = pl.ds(c * span, span)
        return pltpu.make_async_copy(values_hbm.at[block], values.at[block], values_sem.at[c])

    loads[0].start()
    for c in range(rows // span):
        keys_load(c).start()
        values_load(c).start()
    for load in (loads[4], loads[1], loads[2], loads[3]):
        load.start()

    barrier = pltpu.get_barrier_semaphore()

    def greet(k, carry):
        other = lax.rem(me + k, n)
        pl.semaphore_signal(barrier, inc=1, device_id=(other, core), device_id_type=MESH)
        pl.semaphore_signal(barrier, inc=1, device_id=(other, peer), device_id_type=MESH)
        return carry

    lax.fori_loop(1, n, greet, 0)
    pl.semaphore_signal(barrier, inc=1, device_id=(me, peer), device_id_type=MESH)

    start = tokens_ref[...].astype(f32)
    normed_ref[...] = (
        start
        * lax.rsqrt(jnp.mean(start * start, axis=-1, keepdims=True) + 1e-06)
        * attn_gain_ref[...]
    ).astype(jnp.bfloat16)
    loads[0].wait()
    queries = jnp.dot(normed_ref[...], w_query[...], preferred_element_type=f32)
    queries = queries.astype(jnp.bfloat16).astype(f32)
    for h in range(local_heads):
        query_ref[:, h, :] = queries[:, h * head_dim : (h + 1) * head_dim]
    pl.semaphore_wait(barrier, 2 * n - 1)

    def team_copy(source, gathered, sems, origin, other):
        return remote(
            source,
            gathered.at[origin],
            sems.at[0, other],
            sems.at[1, origin],
            team * group_size + other,
            core,
        )

    def send_weights(k, carry):
        other = lax.rem(place + k, group_size)
        team_copy(dense_gate_ref, dense_gate_all, dense_gate_sems, place, other).start()
        team_copy(dense_up_ref, dense_up_all, dense_up_sems, place, other).start()
        team_copy(down_ref, down_all, down_sems, place, other).start()
        return carry

    lax.fori_loop(1, group_size, send_weights, 0)
    dense_gate_all[place] = dense_gate_ref[...]
    dense_up_all[place] = dense_up_ref[...]
    down_all[place] = down_ref[...]

    block_len = min(256, cache_len)
    after_mask = (
        lax.broadcasted_iota(jnp.int32, (block_len, block_len), 0)
        > lax.broadcasted_iota(jnp.int32, (block_len, block_len), 1)
    ).astype(jnp.bfloat16)
    position = lax.broadcasted_iota(jnp.int32, (span * local_heads, block_len), 1)

    head_row = lax.broadcasted_iota(jnp.int32, (local_heads, local_heads), 0)
    head_col = lax.broadcasted_iota(jnp.int32, (local_heads, local_heads), 1)
    bias = jnp.sum(jnp.where(head_row == head_col, bias_ref[...], 0.0), axis=1, keepdims=True)
    lines = span * local_heads
    line_seq = lax.broadcasted_iota(jnp.int32, (lines, rows), 0) // local_heads
    seq_lane = lax.broadcasted_iota(jnp.int32, (lines, rows), 1)
    lengths_row = lengths_ref[...].astype(f32)

    def attend(c, carry):
        keys_load(c).wait()
        for i in range(span):
            s = c * span + i
            score_ref[s] = (
                jnp.dot(query_ref[s].astype(jnp.bfloat16), keys[s], preferred_element_type=f32)
                * head_dim ** (-0.5)
                + bias
            )
        limits = jnp.sum(
            jnp.where(seq_lane == line_seq + c * span, lengths_row, 0.0), axis=1, keepdims=True
        ).astype(jnp.int32)
        later = jnp.zeros((lines, 1), f32)
        for first_pos in range(cache_len - block_len, -1, -block_len):
            columns = slice(first_pos, first_pos + block_len)
            scores = score_ref[pl.ds(c * span, span), :, columns].reshape(lines, block_len)
            visible = position + first_pos < limits
            keep = -(jnp.maximum(scores, 0.0) + jnp.log1p(jnp.exp(-jnp.abs(scores))))
            log_take = scores + keep
            keep = jnp.where(visible, keep, 0.0)
            top = keep.astype(jnp.bfloat16)
            rest = keep - top.astype(f32)
            middle = rest.astype(jnp.bfloat16)
            low = (rest - middle.astype(f32)).astype(jnp.bfloat16)
            sums = jnp.dot(
                jnp.concatenate([top, middle, low], axis=0),
                after_mask,
                preferred_element_type=f32,
            )
            after = sums[:lines] + sums[lines : 2 * lines] + sums[2 * lines :] + later
            later = later + jnp.sum(keep, axis=-1, keepdims=True)
            stick = jnp.where(visible, jnp.exp(log_take + after), 0.0)
            score_ref[pl.ds(c * span, span), :, columns] = stick.reshape(
                span, local_heads, block_len
            )
        values_load(c).wait()
        for i in range(span):
            s = c * span + i
            read_ref[s] = lax.dot_general(
                score_ref[s].astype(jnp.bfloat16),
                values[s],
                (((1,), (1,)), ((), ())),
                preferred_element_type=f32,
            )
        return carry

    lax.fori_loop(0, rows // span, attend, 0)
    heads_out = jnp.concatenate(
        [read_ref[:, h, :] for h in range(local_heads)], axis=1
    ).astype(jnp.bfloat16)
    loads[4].wait()
    attn_mine[...] = jnp.dot(heads_out, w_out[...], preferred_element_type=f32).astype(
        jnp.bfloat16
    )

    swap = remote(attn_mine, attn_peer, pair_sems.at[0], pair_sems.at[1], me, peer)
    swap.start()
    swap.wait()
    attn = attn_mine[...].astype(f32) + attn_peer[...].astype(f32)
    residual = (tokens_ref[...].astype(f32) + attn).astype(jnp.bfloat16)
    res_ref[...] = residual
    wide = residual.astype(f32)
    normed = (
        wide * lax.rsqrt(jnp.mean(wide * wide, axis=-1, keepdims=True) + 1e-06) * gain_ref[...]
    ).astype(jnp.bfloat16)
    norm_all[0, me] = normed[:, :half]
    norm_all[1, me] = normed[:, half:]

    def norm_copy(j, other):
        return remote(
            norm_all.at[core, j],
            norm_all.at[core, j],
            norm_sems.at[0, other],
            norm_sems.at[1, j],
            other,
            core,
        )

    def pass_copy(j, which):
        return remote(
            norm_all.at[which, j],
            norm_all.at[which, j],
            pass_sems.at[0, j],
            pass_sems.at[1, j],
            me,
            peer,
        )

    def send_norm(k, carry):
        norm_copy(me, lax.rem(me + k, n)).start()
        return carry

    lax.fori_loop(1, n, send_norm, 0)

    across = (((1,), (1,)), ((), ()))
    probs = jax.nn.sigmoid(
        lax.dot_general(router_ref[...], normed, across, preferred_element_type=f32)
    )
    expert_total = probs.shape[0]
    expert_row = lax.broadcasted_iota(jnp.int32, (expert_total, rows), 0)
    hits = jnp.zeros((expert_total, rows), f32)
    for k in range(routes_ref.shape[0]):
        hits = jnp.where(routes_ref[k : k + 1, :] == expert_row, 1.0, hits)
    picked = jnp.where(hits > 0.0, probs, 0.0)
    gates = (picked / jnp.sum(picked, axis=0, keepdims=True) * 2.5).T
    expert_index = lax.broadcasted_iota(jnp.int32, (rows, expert_total), 1)
    mix_gate = jax.nn.sigmoid(
        jnp.sum(normed.astype(f32) * mix_ref[...], axis=-1, keepdims=True)
    )

    for weight, target in ((w_key_ref, new_keys_ref), (w_value_ref, new_values_ref)):
        target[...] = lax.dot_general(
            normed_ref[...], weight[...], across, preferred_element_type=f32
        ).astype(jnp.bfloat16)

    def take_norm(k, carry):
        j = lax.rem(me + n - k, n)
        norm_copy(j, me).wait_recv()
        pass_copy(j, core).start()
        return carry

    lax.fori_loop(1, n, take_norm, 0)

    def take_pass(k, carry):
        pass_copy(lax.rem(me + n - k, n), peer).wait_recv()
        return carry

    lax.fori_loop(1, n, take_pass, 0)

    def part_copy(m, other):
        return remote(
            part_send.at[other],
            part_recv.at[m],
            part_sems.at[0, other],
            part_sems.at[1, m],
            other * group_size + place,
            core,
        )

    def back_copy(j, other):
        return remote(
            back_send.at[other],
            back_recv.at[j],
            back_sems.at[0, other],
            back_sems.at[1, j],
            other,
            core,
        )

    def dense_copy(m, other):
        return remote(
            dense_all.at[m],
            dense_all.at[m],
            dense_sems.at[0, other],
            dense_sems.at[1, m],
            other * group_size + place,
            core,
        )

    group = min(n, 16)
    groups = n // group
    block = group * rows

    def take_weights(k, carry):
        other = lax.rem(place + k, group_size)
        team_copy(dense_gate_ref, dense_gate_all, dense_gate_sems, other, place).wait_recv()
        team_copy(dense_up_ref, dense_up_all, dense_up_sems, other, place).wait_recv()
        team_copy(down_ref, down_all, down_sems, other, place).wait_recv()
        return carry

    lax.fori_loop(1, group_size, take_weights, 0)
    features = jnp.concatenate(
        [norm_all[owner, m * group_size + place, :, pl.ds(lane, window)] for m in range(teams)],
        axis=0,
    )
    hidden_cols = dense_gate_ref.shape[1]
    for gathered, columns in (
        (dense_gate_all, slice(0, hidden_cols)),
        (dense_up_all, slice(hidden_cols, 2 * hidden_cols)),
    ):
        value = jnp.dot(
            features, gathered[...].reshape(window, hidden_cols), preferred_element_type=f32
        )
        part_send[:, :, columns] = value.astype(jnp.bfloat16).reshape(teams, rows, hidden_cols)

    def send_part(k, carry):
        part_copy(team, lax.rem(team + k, teams)).start()
        return carry

    lax.fori_loop(1, teams, send_part, 0)

    loads[1].wait()
    loads[2].wait()

    def expert_first(c, carry):
        base = c * group
        low = norm_all[0, pl.ds(base, group)].reshape(block, half)
        high = norm_all[1, pl.ds(base, group)].reshape(block, half)
        gate_rows = jnp.dot(low, w_gate[:half], preferred_element_type=f32) + jnp.dot(
            high, w_gate[half:], preferred_element_type=f32
        )
        up_rows = jnp.dot(low, w_up[:half], preferred_element_type=f32) + jnp.dot(
            high, w_up[half:], preferred_element_type=f32
        )
        hidden_ref[pl.ds(c, 1)] = (jax.nn.silu(gate_rows) * up_rows).astype(jnp.bfloat16)[None]
        return carry

    lax.fori_loop(0, groups, expert_first, 0)

    def take_part(k, total):
        m = lax.rem(team + teams - k, teams)
        part_copy(m, team).wait_recv()
        return total + part_recv[m].astype(f32)

    paired = lax.fori_loop(1, teams, take_part, part_send[team].astype(f32))
    dense_all[team] = (jax.nn.silu(paired[:, :hidden_cols]) * paired[:, hidden_cols:]).astype(
        jnp.bfloat16
    )

    def send_dense(k, carry):
        dense_copy(team, lax.rem(team + k, teams)).start()
        return carry

    lax.fori_loop(1, teams, send_dense, 0)

    loads[3].wait()
    far = pl.ds(pl.multiple_of(peer * half, half), half)
    near = pl.ds(pl.multiple_of(core * half, half), half)

    def expert_far(c, carry):
        value = jnp.dot(hidden_ref[c], w_down[:, far], preferred_element_type=f32)
        other_ref[pl.ds(c * group, group)] = value.astype(jnp.bfloat16).reshape(group, rows, half)
        return carry

    lax.fori_loop(0, groups, expert_far, 0)
    trade = remote(other_ref, peer_ref, pair_sems.at[2], pair_sems.at[3], me, peer)
    trade.start()

    def expert_near(c, carry):
        value = jnp.dot(hidden_ref[c], w_down[:, near], preferred_element_type=f32)
        mine_ref[pl.ds(c * group, group)] = value.astype(jnp.bfloat16).reshape(group, rows, half)
        return carry

    lax.fori_loop(0, groups, expert_near, 0)
    trade.wait()

    def send_back(k, carry):
        other = lax.rem(me + k, n)
        total = mine_ref[other].astype(f32) + peer_ref[other].astype(f32)
        back_send[other] = total.astype(jnp.bfloat16)

        @pl.when(k > 0)
        def _():
            back_copy(me, other).start()

        return carry

    lax.fori_loop(0, n, send_back, 0)

    def take_dense(k, carry):
        dense_copy(lax.rem(team + teams - k, teams), team).wait_recv()
        return carry

    lax.fori_loop(1, teams, take_dense, 0)
    dense_rows = dense_all[...].reshape(teams * rows, hidden_cols)
    columns = [
        jnp.dot(dense_rows, down_all[q], preferred_element_type=f32) for q in range(group_size)
    ]
    cols_send[...] = (
        jnp.concatenate(columns, axis=1).astype(jnp.bfloat16).reshape(cols_send.shape)
    )

    def cols_copy(from_core, m, other, target):
        return remote(
            cols_send.at[other],
            cols_recv.at[from_core, m],
            cols_send_sem.at[other],
            cols_recv_sem.at[from_core, m],
            other * group_size + place,
            target,
        )

    def send_cols(k, carry):
        cols_copy(core, team, lax.rem(team + k, teams), owner).start()
        return carry

    lax.fori_loop(1, teams, send_cols, 0)

    @pl.when(owner == core)
    def _():
        cols_recv[core, team] = cols_send[team]

    @pl.when(owner != core)
    def _():
        cols_copy(core, team, team, peer).start()

    side = teams // 2

    def take_cols(k, carry):
        m = core * side + k

        @pl.when(m != team)
        def _():
            cols_copy(core, m, team, core).wait_recv()

        cols_copy(peer, m, team, core).wait_recv()
        return carry

    lax.fori_loop(0, side, take_cols, 0)
    dense = jnp.concatenate(
        [
            cols_recv[0, core * side + q].astype(f32) + cols_recv[1, core * side + q].astype(f32)
            for q in range(side)
        ],
        axis=1,
    )
    total = res_ref[:, near].astype(f32) + mix_gate * dense

    def take_back(k, total):
        j = lax.rem(me + n - k, n)

        @pl.when(k > 0)
        def _():
            back_copy(j, me).wait_recv()

        @pl.when(k == 0)
        def _():
            back_recv[me] = back_send[me]

        gate = jnp.sum(jnp.where(expert_index == j, gates, 0.0), axis=-1, keepdims=True)
        return total + gate * back_recv[j].astype(f32)

    out_ref[...] = lax.fori_loop(0, n, take_back, total).astype(jnp.bfloat16)

    def drain(k, carry):
        other = lax.rem(me + k, n)
        norm_copy(me, other).wait_send()
        pass_copy(other, core).wait_send()
        back_copy(me, other).wait_send()
        return carry

    lax.fori_loop(1, n, drain, 0)

    def drain_team(k, carry):
        other = lax.rem(place + k, group_size)
        team_copy(dense_gate_ref, dense_gate_all, dense_gate_sems, place, other).wait_send()
        team_copy(dense_up_ref, dense_up_all, dense_up_sems, place, other).wait_send()
        team_copy(down_ref, down_all, down_sems, place, other).wait_send()
        return carry

    lax.fori_loop(1, group_size, drain_team, 0)

    def drain_dense(k, carry):
        other = lax.rem(team + k, teams)
        part_copy(team, other).wait_send()
        dense_copy(team, other).wait_send()
        cols_copy(core, team, other, owner).wait_send()
        return carry

    lax.fori_loop(1, teams, drain_dense, 0)

    @pl.when(owner != core)
    def _():
        cols_copy(core, team, team, peer).wait_send()


def shards(
    n,
    tokens,
    lengths,
    attn_gain,
    w_query,
    w_key,
    w_value,
    head_bias,
    key_cache,
    value_cache,
    w_attn_out,
    ffn_gain,
    w_router,
    routes,
    w_dense_gate,
    w_dense_up,
    w_dense_down,
    dense_mix,
    w_expert_gate,
    w_expert_up,
    w_expert_down,
):
    rows, model = tokens.shape
    half = model // 2
    width, hidden_cols = w_dense_gate.shape
    group_size = min(n, max(4, 128 // width))
    teams = n // group_size
    window = width * group_size
    seq_count, local_kv, head_dim, cache_len = key_cache.shape
    local_heads = head_bias.shape[0]
    keys = key_cache.reshape(seq_count, head_dim, cache_len)
    values = value_cache.reshape(seq_count, head_dim, cache_len)
    w_gate, w_up, w_down = w_expert_gate[0], w_expert_up[0], w_expert_down[0]
    expert_hidden = w_gate.shape[1]
    bf16, f32 = jnp.bfloat16, jnp.float32
    block = min(n, 16) * rows
    vmem = pl.BlockSpec(memory_space=pltpu.VMEM)
    anywhere = pl.BlockSpec(memory_space=pltpu.HBM)
    dma = pltpu.SemaphoreType.DMA
    return pl.pallas_call(
        functools.partial(whole_layer, n, group_size),
        out_shape=(
            jax.ShapeDtypeStruct((rows, half), bf16),
            jax.ShapeDtypeStruct((rows, w_key.shape[1]), bf16),
            jax.ShapeDtypeStruct((rows, w_value.shape[1]), bf16),
        ),
        in_specs=[vmem] * 13 + [anywhere] * 7,
        out_specs=(vmem, vmem, vmem),
        scratch_shapes=[
            pltpu.VMEM(w_query.shape, bf16),
            pltpu.VMEM(w_attn_out.shape, bf16),
            pltpu.VMEM(w_gate.shape, bf16),
            pltpu.VMEM(w_up.shape, bf16),
            pltpu.VMEM(w_down.shape, bf16),
            pltpu.VMEM(keys.shape, bf16),
            pltpu.VMEM(values.shape, bf16),
            dma((5,)),
            dma((rows // 4,)),
            dma((rows // 4,)),
            pltpu.VMEM((rows, local_heads, head_dim), f32),
            pltpu.VMEM((rows, local_heads, cache_len), f32),
            pltpu.VMEM((rows, local_heads, head_dim), f32),
            pltpu.VMEM((rows, model), bf16),
            pltpu.VMEM((group_size, width, hidden_cols), bf16),
            pltpu.VMEM((group_size, width, hidden_cols), bf16),
            pltpu.VMEM((group_size, hidden_cols, width), bf16),
            pltpu.VMEM((rows, model), bf16),
            pltpu.VMEM((rows, model), bf16),
            pltpu.VMEM((rows, model), bf16),
            pltpu.VMEM((2, n, rows, half), bf16),
            pltpu.VMEM((teams, rows, 2 * hidden_cols), bf16),
            pltpu.VMEM((teams, rows, 2 * hidden_cols), bf16),
            pltpu.VMEM((n * rows // block, block, expert_hidden), bf16),
            pltpu.VMEM((teams, rows, hidden_cols), bf16),
            pltpu.VMEM((teams, rows, window), bf16),
            pltpu.VMEM((2, teams, rows, window), bf16),
            pltpu.VMEM((n, rows, half), bf16),
            pltpu.VMEM((n, rows, half), bf16),
            pltpu.VMEM((n, rows, half), bf16),
            pltpu.VMEM((n, rows, half), bf16),
            pltpu.VMEM((n, rows, half), bf16),
            dma((4,)),
            dma((2, group_size)),
            dma((2, group_size)),
            dma((2, group_size)),
            dma((2, n)),
            dma((2, n)),
            dma((2, teams)),
            dma((2, teams)),
            dma((teams,)),
            dma((2, teams)),
            dma((2, n)),
        ],
        compiler_params=pltpu.CompilerParams(
            collective_id=0, has_side_effects=True, vmem_limit_bytes=63 * 1024 * 1024
        ),
        name="whole_layer",
    )(
        tokens,
        attn_gain.reshape(1, model),
        lengths.reshape(1, seq_count),
        head_bias.reshape(1, local_heads),
        w_key.T,
        w_value.T,
        ffn_gain.reshape(1, model),
        w_router.T,
        routes.T,
        dense_mix.reshape(1, model),
        w_dense_gate,
        w_dense_up,
        w_dense_down,
        w_query,
        w_attn_out,
        w_gate,
        w_up,
        w_down,
        keys,
        values,
    )


def solution(mesh):
    return jax.shard_map(
        functools.partial(shards, mesh.shape["ep"]),
        mesh=mesh,
        in_specs=(
            P("ep", None),
            P("ep"),
            P(),
            P(None, "tp"),
            P(None, "tp"),
            P(None, "tp"),
            P("tp"),
            P("ep", "tp", None, None),
            P("ep", "tp", None, None),
            P("tp", None),
            P(),
            P(),
            P("ep", None),
            P("ep", "tp"),
            P("ep", "tp"),
            P("tp", "ep"),
            P(),
            P("ep", None, "tp"),
            P("ep", None, "tp"),
            P("ep", "tp", None),
        ),
        out_specs=(P("ep", "tp"), P("ep", "tp"), P("ep", "tp")),
        check_vma=False,
    )
```
